32 devices in a mesh: rep: 2 (over x), fs: 8 (over z, y), tp: 2 (over core).
Axes of the slice: x: 2, y: 2, z: 4, core: 2. Of those that a mesh axis runs over, the one named last changes fastest.
Arguments:
- stream: bfloat16 [16, 512, 2048], P(('rep', 'fs'), None, 'tp'), may hold values from -60 to 60
- pre_gain_mix: float32 [2048], P('tp'), may hold values from 0.1 to 1.9
- value_weight: bfloat16 [2048, 2048], P('fs', 'tp'), may hold values from -0.125 to 0.125
- gate_weight: bfloat16 [2048, 2048], P('fs', 'tp'), may hold values from -0.125 to 0.125
- mix_kernel: bfloat16 [31, 2048], P(None, 'tp'), may hold values from -2 to 2
- mix_bias: float32 [2048], P('tp'), may hold values from -2 to 8
- chan_gain: float32 [2048], P('tp'), may hold values from 0.1 to 1.9
- proj_weight: bfloat16 [2048, 2048], P('fs', 'tp'), may hold values from -2 to 2
- post_gain_mix: float32 [2048], P('tp'), may hold values from 0.1 to 1.9
- pre_gain_ffn: float32 [2048], P('tp'), may hold values from 0.1 to 1.9
- up_gate_weight: bfloat16 [2048, 2816], P('fs', 'tp'), may hold values from -0.125 to 0.125
- up_value_weight: bfloat16 [2048, 2816], P('fs', 'tp'), may hold values from -0.125 to 0.125
- gate_kernel: bfloat16 [3, 2816], P(None, 'tp'), may hold values from -2.5 to 2.5
- value_kernel: bfloat16 [3, 2816], P(None, 'tp'), may hold values from -2.5 to 2.5
- down_weight: bfloat16 [2048, 2816], P('fs', 'tp'), may hold values from -2 to 2
- post_gain_ffn: float32 [2048], P('tp'), may hold values from 0.1 to 1.9
Outputs:
- out_stream: bfloat16 [16, 512, 2048], P(('rep', 'fs'), None, 'tp')
The draws below stay inside these ranges and needn't reach their ends.
All inputs are finite; a program needn't handle non-finite values.
Results may differ from the reference program's by a relative error of at most 0.014.
Values may be sent and summed in bfloat16 or wider, within the bound.
A program may use at most 128 MiB of HBM per device.

```python
import math
import jax
import jax.numpy as jnp
from jax import lax

D = 2048
F = 2816
KW = 31
FW = 3
LEN = 512
SEQS = 16
N_TP = 2


def channel_ramp(count, top):
    return jnp.exp(jnp.linspace(0.0, math.log(top), count)).astype(jnp.float32)


def draw_stream(key, part):
    key = jax.random.fold_in(key, 11)
    values = jnp.clip(jax.random.normal(key, (SEQS, LEN, D), jnp.float32), -4.0, 4.0)
    return (values * channel_ramp(D, 3.0)).astype(jnp.bfloat16)


def draw_mix_kernel(key, part):
    key = jax.random.fold_in(key, 23)
    values = jnp.clip(jax.random.normal(key, (KW, D), jnp.float32), -3.0, 3.0)
    return (values * KW ** (-0.5) * channel_ramp(D, 3.0)).astype(jnp.bfloat16)


def draw_mix_bias(key, part):
    key = jax.random.fold_in(key, 31)
    rough = jnp.clip(jax.random.normal(key, (D,), jnp.float32), -3.0, 3.0) * 0.5
    return (rough + jnp.linspace(0.0, 3.0, D)).astype(jnp.float32)


def draw_proj_weight(key, part):
    key = jax.random.fold_in(key, 37)
    values = jnp.clip(jax.random.normal(key, (D, D), jnp.float32), -3.0, 3.0)
    return (values * D ** (-0.5) * channel_ramp(D, 3.0)[:, None]).astype(jnp.bfloat16)


def draw_down_weight(key, part):
    key = jax.random.fold_in(key, 53)
    values = jnp.clip(jax.random.normal(key, (D, F), jnp.float32), -3.0, 3.0)
    return (values * F ** (-0.5) * channel_ramp(D, 3.0)[:, None]).astype(jnp.bfloat16)


def block_levels(own_key, dims, pieces, low, high):
    def one(dim, blocks):
        heights = jax.random.uniform(jax.random.fold_in(jax.random.fold_in(own_key, 6), dim), (blocks,), jnp.float32, low / len(pieces), high / len(pieces))
        return jnp.repeat(jnp.exp(heights), dims[dim] // blocks).reshape((-1,) + (1,) * (len(dims) - dim - 1))

    factor_of = one(*pieces[0])
    for cut in pieces[1:]:
        factor_of = factor_of * one(*cut)
    return factor_of


def normal_values(own_key, dims, scale, most, cuts=(), kind=jnp.bfloat16):
    result = jax.random.normal(own_key, dims, jnp.float32) * scale
    if len(cuts) > 0:
        result = block_levels(own_key, dims, cuts, -0.22, 0.18) * result
    return jnp.clip(result, min=-most, max=most).astype(kind)


def setup_inputs(seed: int = 0) -> dict:
    seeds = jax.random.split(jax.random.key(seed), 17)
    stream = draw_stream(jax.random.fold_in(seeds[16], 71), 0)
    pre_gain_mix = jnp.clip(1.0 + 0.18 * jax.random.normal(seeds[1], (D,), jnp.float32), 0.1, 1.9)
    value_weight = normal_values(seeds[2], (D, D), D ** -0.5, 0.125, ((0, 8), (1, 2)))
    gate_weight = normal_values(seeds[3], (D, D), D ** -0.5, 0.125, ((0, 8), (1, 2)))
    mix_kernel = draw_mix_kernel(jax.random.fold_in(seeds[16], 71), 0)
    mix_bias = draw_mix_bias(jax.random.fold_in(seeds[16], 71), 0)
    chan_gain = jnp.clip(1.0 + 0.18 * jax.random.normal(seeds[6], (D,), jnp.float32), 0.1, 1.9)
    proj_weight = draw_proj_weight(jax.random.fold_in(seeds[16], 71), 0)
    post_gain_mix = jnp.clip(1.0 + 0.18 * jax.random.normal(seeds[8], (D,), jnp.float32), 0.1, 1.9)
    pre_gain_ffn = jnp.clip(1.0 + 0.18 * jax.random.normal(seeds[9], (D,), jnp.float32), 0.1, 1.9)
    up_gate_weight = normal_values(seeds[10], (D, F), D ** -0.5, 0.125, ((0, 8), (1, 2)))
    up_value_weight = normal_values(seeds[11], (D, F), D ** -0.5, 0.125, ((0, 8), (1, 2)))
    gate_kernel = normal_values(seeds[12], (FW, F), 0.577, 2.5, ((1, 2),))
    value_kernel = normal_values(seeds[13], (FW, F), 0.577, 2.5, ((1, 2),))
    down_weight = draw_down_weight(jax.random.fold_in(seeds[16], 71), 0)
    post_gain_ffn = jnp.clip(1.0 + 0.18 * jax.random.normal(seeds[15], (D,), jnp.float32), 0.1, 1.9)
    return dict(stream=stream, pre_gain_mix=pre_gain_mix, value_weight=value_weight, gate_weight=gate_weight, mix_kernel=mix_kernel, mix_bias=mix_bias, chan_gain=chan_gain, proj_weight=proj_weight, post_gain_mix=post_gain_mix, pre_gain_ffn=pre_gain_ffn, up_gate_weight=up_gate_weight, up_value_weight=up_value_weight, gate_kernel=gate_kernel, value_kernel=value_kernel, down_weight=down_weight, post_gain_ffn=post_gain_ffn)


EPS = 1e-06

def rms_apply(values, gain_vector):
    values32 = values.astype(jnp.float32)
    inverse_rms = lax.rsqrt(lax.optimization_barrier(jnp.mean(values32 * values32, axis=-1, keepdims=True)) + EPS)
    return values32 * inverse_rms * gain_vector

def causal_conv(sequence, kernel):
    taps = kernel.shape[0]
    length = sequence.shape[0]
    padded = jnp.pad(sequence.astype(jnp.float32), ((taps - 1, 0), (0, 0)))
    running = jnp.zeros(sequence.shape, jnp.float32)
    for offset in range(taps):
        running = running + kernel[offset].astype(jnp.float32) * padded[offset:offset + length]
    return running

def split_product(activated, weight_rows):
    block_width = activated.shape[1] // N_TP
    running = jnp.zeros((activated.shape[0], weight_rows.shape[0]), jnp.float32)
    for block_index in range(N_TP):
        lower = block_index * block_width
        partial_sum = lax.dot_general(activated[:, lower:lower + block_width], weight_rows[:, lower:lower + block_width], (((1,), (1,)), ((), ())), preferred_element_type=jnp.float32)
        rounded = lax.optimization_barrier(partial_sum.astype(jnp.bfloat16))
        running = running + rounded.astype(jnp.float32)
    return running

def reference(stream, pre_gain_mix, value_weight, gate_weight, mix_kernel, mix_bias, chan_gain, proj_weight, post_gain_mix, pre_gain_ffn, up_gate_weight, up_value_weight, gate_kernel, value_kernel, down_weight, post_gain_ffn):

    def one_sequence(sequence):
        normed = rms_apply(sequence, pre_gain_mix).astype(jnp.bfloat16)
        value_part = jnp.dot(normed, value_weight, preferred_element_type=jnp.float32)
        gate_part = jnp.dot(normed, gate_weight, preferred_element_type=jnp.float32)
        glu = (value_part * jax.nn.sigmoid(gate_part)).astype(jnp.bfloat16)
        convolved = causal_conv(glu, mix_kernel) + mix_bias
        chan_mean = lax.optimization_barrier(jnp.mean(convolved, axis=-1, keepdims=True))
        centred = convolved - chan_mean
        chan_var = lax.optimization_barrier(jnp.mean(centred * centred, axis=-1, keepdims=True))
        activated = jax.nn.silu(centred * lax.rsqrt(chan_var + EPS) * chan_gain).astype(jnp.bfloat16)
        mixed = split_product(activated, proj_weight).astype(jnp.bfloat16)
        middle = (sequence.astype(jnp.float32) + rms_apply(mixed, post_gain_mix)).astype(jnp.bfloat16)
        normed_ffn = rms_apply(middle, pre_gain_ffn).astype(jnp.bfloat16)
        up_gate = jnp.dot(normed_ffn, up_gate_weight, preferred_element_type=jnp.float32).astype(jnp.bfloat16)
        up_value = jnp.dot(normed_ffn, up_value_weight, preferred_element_type=jnp.float32).astype(jnp.bfloat16)
        hidden = (jax.nn.silu(causal_conv(up_gate, gate_kernel)) * causal_conv(up_value, value_kernel)).astype(jnp.bfloat16)
        ffn_out = split_product(hidden, down_weight).astype(jnp.bfloat16)
        return (middle.astype(jnp.float32) + rms_apply(ffn_out, post_gain_ffn)).astype(jnp.bfloat16)
    return lax.map(one_sequence, stream)
```

```python
import jax
import jax.numpy as jnp
from jax import lax
from jax.sharding import PartitionSpec as P

EPS = 1e-06


def swap(values, axis):
    count = lax.axis_size(axis)
    if count == 1:
        return values
    return lax.ppermute(values, axis, [(i, i ^ 1) for i in range(count)])


def pass_on(values, inner):
    count = lax.axis_size("fs")
    return lax.ppermute(values, "fs", [(i, (i + inner) % count) for i in range(count)])


def own_part(values, dim):
    size = values.shape[dim] // lax.axis_size("rep")
    return lax.dynamic_slice_in_dim(values, lax.axis_index("rep") * size, size, axis=dim)


def gather_shards(piece, pair_first):
    count, rows = lax.axis_size("fs"), piece.shape[0]
    inner = 2 if count % 2 == 0 else 1
    outer = count // inner
    index = lax.axis_index("fs")
    high, low = index // inner, index % inner
    buffer = jnp.zeros((count * rows, piece.shape[1]), piece.dtype)

    def put(buffer, block, step, low_at):
        owner = lax.rem(high - step + outer, outer) * inner + low_at
        return lax.dynamic_update_slice_in_dim(buffer, block, owner * rows, axis=0)

    mine = piece
    other = swap(piece, "fs") if inner == 2 else None
    for step in range(outer):
        buffer = put(buffer, mine, step, low)
        if inner == 2:
            buffer = put(buffer, other, step, 1 - low)
        if step < outer - 1:
            mine = pass_on(mine, inner)
            if inner == 2:
                other = pass_on(other, inner) if pair_first else swap(mine, "fs")
    return buffer


def square_total(values32):
    return lax.psum(jnp.sum(values32 * values32, axis=-1), "tp")


def rms_apply(values32, gain_vector):
    row_width = values32.shape[-1] * lax.axis_size("tp")
    inverse_rms = lax.rsqrt(square_total(values32) / row_width + EPS)
    return values32 * inverse_rms[..., None] * gain_vector


def ordered(own, other, axis, dim):
    first = lax.axis_index(axis) == 0
    return jnp.where(
        first, jnp.concatenate([own, other], axis=dim), jnp.concatenate([other, own], axis=dim)
    )


def gather_rows(normed):
    pair = jnp.stack([normed, swap(normed, "rep")]) if lax.axis_size("rep") > 1 else normed[None]
    return ordered(pair, swap(pair, "tp"), "tp", 2)


def column_total(terms):
    width = terms.shape[2] // lax.axis_size("tp")
    lower, upper = terms[:, :, :width], terms[:, :, width:]
    first = lax.axis_index("tp") == 0
    kept = jnp.where(first, lower, upper)
    sent = jnp.where(first, upper, lower).astype(jnp.bfloat16)
    half = kept + swap(sent, "tp").astype(jnp.float32)
    if half.shape[0] == 1:
        return half[0]
    return half[0] + swap(half[1].astype(jnp.bfloat16), "rep").astype(jnp.float32)


def pair_order(sums):
    return jnp.where(lax.axis_index("rep") % 2 == 0, sums, sums[::-1])


def causal_conv(sequences, kernel):
    taps = kernel.shape[0]
    length = sequences.shape[1]
    padded = jnp.pad(sequences.astype(jnp.float32), ((0, 0), (taps - 1, 0), (0, 0)))
    running = jnp.zeros(sequences.shape, jnp.float32)
    for offset in range(taps):
        running = running + kernel[offset].astype(jnp.float32) * padded[:, offset : offset + length]
    return running


def contract(activated, weight_rows):
    return lax.dot_general(
        activated, weight_rows, (((2,), (1,)), ((), ())), preferred_element_type=jnp.float32
    )


def per_device(
    stream,
    pre_gain_mix,
    value_weight,
    gate_weight,
    mix_kernel,
    mix_bias,
    chan_gain,
    proj_weight,
    post_gain_mix,
    pre_gain_ffn,
    up_gate_weight,
    up_value_weight,
    gate_kernel,
    value_kernel,
    down_weight,
    post_gain_ffn,
):
    sequence = stream[0].astype(jnp.float32)
    mix_pair = gather_shards(
        jnp.concatenate([own_part(value_weight, 1), own_part(gate_weight, 1)], axis=1), False
    )
    proj_rows = gather_shards(own_part(proj_weight, 1), True)
    up_pair = gather_shards(
        jnp.concatenate([own_part(up_gate_weight, 1), own_part(up_value_weight, 1)], axis=1), False
    )
    down_rows = gather_shards(own_part(down_weight, 1), False)

    normed = rms_apply(sequence, pre_gain_mix).astype(jnp.bfloat16)
    whole_rows = gather_rows(normed)
    both = jnp.dot(whole_rows, mix_pair, preferred_element_type=jnp.float32)
    width = both.shape[2] // 2
    glu = (both[:, :, :width] * jax.nn.sigmoid(both[:, :, width:])).astype(jnp.bfloat16)
    convolved = causal_conv(glu, own_part(mix_kernel, 1)) + own_part(mix_bias, 0)
    groups = ("rep", "tp")
    row_width = width * lax.axis_size("rep") * lax.axis_size("tp")
    chan_mean = pair_order(lax.psum(pair_order(jnp.sum(convolved, axis=2)), groups)) / row_width
    centred = convolved - chan_mean[..., None]
    square_sums = lax.psum(pair_order(jnp.sum(centred * centred, axis=2)), groups)
    chan_var = pair_order(square_sums) / row_width
    activated = jax.nn.silu(
        centred * lax.rsqrt(chan_var + EPS)[..., None] * own_part(chan_gain, 0)
    ).astype(jnp.bfloat16)
    mixed = column_total(contract(activated, proj_rows)).astype(jnp.bfloat16)
    middle = (sequence + rms_apply(mixed.astype(jnp.float32), post_gain_mix)).astype(jnp.bfloat16)
    middle32 = middle.astype(jnp.float32)
    normed_ffn = rms_apply(middle32, pre_gain_ffn).astype(jnp.bfloat16)
    up = jnp.dot(gather_rows(normed_ffn), up_pair, preferred_element_type=jnp.float32)
    up = up.astype(jnp.bfloat16)
    hidden_width = up.shape[2] // 2
    hidden = (
        jax.nn.silu(causal_conv(up[:, :, :hidden_width], own_part(gate_kernel, 1)))
        * causal_conv(up[:, :, hidden_width:], own_part(value_kernel, 1))
    ).astype(jnp.bfloat16)
    ffn_out = column_total(contract(hidden, down_rows)).astype(jnp.bfloat16)
    result = (middle32 + rms_apply(ffn_out.astype(jnp.float32), post_gain_ffn)).astype(jnp.bfloat16)
    return result[None]


def solution(mesh):
    placed = (
        P(("rep", "fs"), None, "tp"),
        P("tp"),
        P("fs", "tp"),
        P("fs", "tp"),
        P(None, "tp"),
        P("tp"),
        P("tp"),
        P("fs", "tp"),
        P("tp"),
        P("tp"),
        P("fs", "tp"),
        P("fs", "tp"),
        P(None, "tp"),
        P(None, "tp"),
        P("fs", "tp"),
        P("tp"),
    )
    return jax.shard_map(
        per_device,
        mesh=mesh,
        in_specs=placed,
        out_specs=P(("rep", "fs"), None, "tp"),
        check_vma=False,
    )
```

```python
import jax
import jax.numpy as jnp
from jax import lax
from jax.sharding import PartitionSpec as P

EPS = 1e-06


def swap(values, axis):
    count = lax.axis_size(axis)
    if count == 1:
        return values
    return lax.ppermute(values, axis, [(i, i ^ 1) for i in range(count)])


def pass_on(values, inner):
    count = lax.axis_size("fs")
    return lax.ppermute(values, "fs", [(i, (i + inner) % count) for i in range(count)])


def own_part(values, dim):
    size = values.shape[dim] // lax.axis_size("rep")
    return lax.dynamic_slice_in_dim(values, lax.axis_index("rep") * size, size, axis=dim)


def gather_shards(piece, pair_first):
    if pair_first is None:
        return lax.all_gather(piece, "fs", axis=0, tiled=True)
    count, rows = lax.axis_size("fs"), piece.shape[0]
    inner = 2 if count % 2 == 0 else 1
    outer = count // inner
    index = lax.axis_index("fs")
    high, low = index // inner, index % inner
    buffer = jnp.zeros((count * rows, piece.shape[1]), piece.dtype)

    def put(buffer, block, step, low_at):
        owner = lax.rem(high - step + outer, outer) * inner + low_at
        return lax.dynamic_update_slice_in_dim(buffer, block, owner * rows, axis=0)

    mine = piece
    other = swap(piece, "fs") if inner == 2 else None
    for step in range(outer):
        buffer = put(buffer, mine, step, low)
        if inner == 2:
            buffer = put(buffer, other, step, 1 - low)
        if step < outer - 1:
            mine = pass_on(mine, inner)
            if inner == 2:
                other = pass_on(other, inner) if pair_first else swap(mine, "fs")
    return buffer


def square_total(values32):
    return lax.psum(jnp.sum(values32 * values32, axis=-1), "tp")


def rms_apply(values32, gain_vector):
    row_width = values32.shape[-1] * lax.axis_size("tp")
    inverse_rms = lax.rsqrt(square_total(values32) / row_width + EPS)
    return values32 * inverse_rms[..., None] * gain_vector


def ordered(own, other, axis, dim):
    first = lax.axis_index(axis) == 0
    return jnp.where(
        first, jnp.concatenate([own, other], axis=dim), jnp.concatenate([other, own], axis=dim)
    )


def join_pair(rows):
    return jnp.stack([rows, swap(rows, "rep")]) if lax.axis_size("rep") > 1 else rows[None]


def whole_width(rows):
    return ordered(rows, swap(rows, "tp"), "tp", 2)


def column_total(terms):
    width = terms.shape[2] // lax.axis_size("tp")
    lower, upper = terms[:, :, :width], terms[:, :, width:]
    first = lax.axis_index("tp") == 0
    kept = jnp.where(first, lower, upper)
    sent = jnp.where(first, upper, lower).astype(jnp.bfloat16)
    half = kept + swap(sent, "tp").astype(jnp.float32)
    if half.shape[0] == 1:
        return half[0]
    return half[0] + swap(half[1].astype(jnp.bfloat16), "rep").astype(jnp.float32)


def pair_order(sums):
    return jnp.where(lax.axis_index("rep") % 2 == 0, sums, sums[::-1])


def causal_conv(sequences, kernel):
    taps = kernel.shape[0]
    length = sequences.shape[1]
    padded = jnp.pad(sequences.astype(jnp.float32), ((0, 0), (taps - 1, 0), (0, 0)))
    running = jnp.zeros(sequences.shape, jnp.float32)
    for offset in range(taps):
        running = running + kernel[offset].astype(jnp.float32) * padded[:, offset : offset + length]
    return running


def contract(activated, weight_rows):
    return lax.dot_general(
        activated, weight_rows, (((2,), (1,)), ((), ())), preferred_element_type=jnp.float32
    )


def per_device(
    stream,
    pre_gain_mix,
    value_weight,
    gate_weight,
    mix_kernel,
    mix_bias,
    chan_gain,
    proj_weight,
    post_gain_mix,
    pre_gain_ffn,
    up_gate_weight,
    up_value_weight,
    gate_kernel,
    value_kernel,
    down_weight,
    post_gain_ffn,
):
    sequence = stream[0].astype(jnp.float32)
    mix_pair = gather_shards(
        jnp.concatenate([own_part(value_weight, 1), own_part(gate_weight, 1)], axis=1), False
    )
    proj_rows = gather_shards(own_part(proj_weight, 1), None)
    up_pair = gather_shards(
        jnp.concatenate([own_part(up_gate_weight, 1), own_part(up_value_weight, 1)], axis=1), None
    )
    down_rows = gather_shards(own_part(down_weight, 1), None)

    pair = join_pair(stream[0]).astype(jnp.float32)
    normed = rms_apply(pair, pre_gain_mix).astype(jnp.bfloat16)
    whole_rows = whole_width(normed)
    both = jnp.dot(whole_rows, mix_pair, preferred_element_type=jnp.float32)
    width = both.shape[2] // 2
    glu = (both[:, :, :width] * jax.nn.sigmoid(both[:, :, width:])).astype(jnp.bfloat16)
    convolved = causal_conv(glu, own_part(mix_kernel, 1)) + own_part(mix_bias, 0)
    own_mean = jnp.mean(convolved, axis=2)
    own_squares = jnp.sum((convolved - own_mean[..., None]) ** 2, axis=2)
    stats = jnp.stack([pair_order(own_mean), pair_order(own_squares)])
    stats = lax.all_gather(stats, ("rep", "tp"), axis=0)
    mean_all = jnp.mean(stats[:, 0], axis=0)
    spread = jnp.sum((stats[:, 0] - mean_all) ** 2, axis=0) * width
    variance = (jnp.sum(stats[:, 1], axis=0) + spread) / (width * stats.shape[0])
    chan_mean, chan_var = pair_order(mean_all), pair_order(variance)
    centred = convolved - chan_mean[..., None]
    activated = jax.nn.silu(
        centred * lax.rsqrt(chan_var + EPS)[..., None] * own_part(chan_gain, 0)
    ).astype(jnp.bfloat16)
    mixed = column_total(contract(activated, proj_rows)).astype(jnp.bfloat16)
    middle = (sequence + rms_apply(mixed.astype(jnp.float32), post_gain_mix)).astype(jnp.bfloat16)
    middle32 = middle.astype(jnp.float32)
    normed_ffn = rms_apply(middle32, pre_gain_ffn).astype(jnp.bfloat16)
    up = jnp.dot(whole_width(join_pair(normed_ffn)), up_pair, preferred_element_type=jnp.float32)
    up = up.astype(jnp.bfloat16)
    hidden_width = up.shape[2] // 2
    hidden = (
        jax.nn.silu(causal_conv(up[:, :, :hidden_width], own_part(gate_kernel, 1)))
        * causal_conv(up[:, :, hidden_width:], own_part(value_kernel, 1))
    ).astype(jnp.bfloat16)
    ffn_out = column_total(contract(hidden, down_rows)).astype(jnp.bfloat16)
    result = (middle32 + rms_apply(ffn_out.astype(jnp.float32), post_gain_ffn)).astype(jnp.bfloat16)
    return result[None]


def solution(mesh):
    placed = (
        P(("rep", "fs"), None, "tp"),
        P("tp"),
        P("fs", "tp"),
        P("fs", "tp"),
        P(None, "tp"),
        P("tp"),
        P("tp"),
        P("fs", "tp"),
        P("tp"),
        P("tp"),
        P("fs", "tp"),
        P("fs", "tp"),
        P(None, "tp"),
        P(None, "tp"),
        P("fs", "tp"),
        P("tp"),
    )
    return jax.shard_map(
        per_device,
        mesh=mesh,
        in_specs=placed,
        out_specs=P(("rep", "fs"), None, "tp"),
        check_vma=False,
    )
```
